32 devices in a mesh: sp: 8 (over z, y), tp: 4 (over x, core).
Axes of the slice: x: 2, y: 2, z: 4, core: 2. Of those that a mesh axis runs over, the one named last changes fastest.
Arguments:
- queries: bfloat16 [1536, 1024], P('sp', 'tp'), may hold values from -0.75 to 0.75
- key_vectors: bfloat16 [1536, 1024], P('sp', 'tp'), may hold values from -0.75 to 0.75
- values_in: bfloat16 [1536, 2048], P('sp', 'tp'), may hold values from -0.75 to 0.75
- log_decay: float32 [1536, 1024], P('sp', 'tp'), may hold values from -1 to 0
- mixed_heads: bfloat16 [1536, 2048], P('sp', 'tp'), may hold values from -6 to 6
- out_proj: bfloat16 [2048, 2048], P('tp'), may hold values from -0.125 to 0.125
- layer_input: bfloat16 [1536, 2048], P('sp'), may hold values from -6 to 6
- cotangent: bfloat16 [1536, 2048], P('sp'), may hold values from -6 to 6
- routes: int32 [1536, 2], P('sp'), may hold values from 0 to 15, all different within a row; in each aligned block of 192 rows (0 to 191, 192 to 383, ...) at most 48 rows name the same one
- route_weight: float32 [1536, 2], P('sp'), may hold values from 0.25 to 2
- gate_weight: bfloat16 [16, 2048, 1024], P('sp', None, 'tp'), may hold values from -0.125 to 0.125
- up_weight: bfloat16 [16, 2048, 1024], P('sp', None, 'tp'), may hold values from -0.125 to 0.125
- down_weight: bfloat16 [16, 1024, 2048], P('sp', 'tp'), may hold values from -0.1875 to 0.1875
Outputs:
- grad_gate: float32 [16, 2048, 1024], P('sp', None, 'tp')
- grad_up: float32 [16, 2048, 1024], P('sp', None, 'tp')
- grad_down: float32 [16, 1024, 2048], P('sp', 'tp')
- grad_proj: float32 [2048, 2048], P('sp', 'tp')
- grad_query: float32 [1536, 1024], P('sp', 'tp')
- grad_key: float32 [1536, 1024], P('sp', 'tp')
- grad_value: float32 [1536, 2048], P('sp', 'tp')
- grad_decay: float32 [1536, 1024], P('sp', 'tp')
The draws below stay inside these ranges and needn't reach their ends.
Inputs may be any that keep to these rules, and one draw needn't show every extreme that they name: `routes`: in each aligned block of 192 tokens no expert is named by more than 48 pairs, and in some block one expert is named by exactly 48 pairs; the 2 experts of a token differ.
All inputs are finite; a program needn't handle non-finite values.
Results may differ from the reference program's by a relative error of at most 0.015.
Values may be sent and summed in bfloat16 or wider, within the bound.
A program may use at most 192 MiB of HBM per device.

```python
import math
import jax
import jax.numpy as jnp
import numpy as np
from jax import lax

D = 2048
HEADS = 8
DK = 128
DV = 256
FE = 1024
TOP = 2
TOK_DEV = 192
EXPERTS = 16
STREAM_LENGTH = 1536
CAP = 48
N_TP = 4


def draw_log_decay(key, part):
    lookup_entries = jax.random.split(key, 7)
    feature_total = HEADS * DK
    fast_share = 0.5
    fast = jax.random.bernoulli(lookup_entries[0], fast_share, (feature_total,))
    fast_rate = jnp.exp(jax.random.uniform(lookup_entries[1], (feature_total,), jnp.float32, jnp.log(1.0 / 50.0), jnp.log(1.0 / 30.0)))
    slow_rate = jnp.exp(jax.random.uniform(lookup_entries[2], (feature_total,), jnp.float32, jnp.log(0.05), jnp.log(0.25))) / STREAM_LENGTH
    rate = jnp.where(fast, fast_rate, slow_rate)
    blocks = STREAM_LENGTH // TOK_DEV
    block_factor = jnp.exp(jax.random.uniform(lookup_entries[3], (blocks, 1, 1), jnp.float32, -0.7, 0.7))
    rough = jnp.exp(jax.random.uniform(lookup_entries[4], (blocks, TOK_DEV, feature_total), jnp.float32, -0.4, 0.4))
    stable_mode = -(rate[None, None, :] * block_factor * rough).reshape(STREAM_LENGTH, feature_total)
    spike_location = jax.random.randint(lookup_entries[5], (3,), 0, STREAM_LENGTH)
    spike_surcharge = jax.random.uniform(lookup_entries[6], (feature_total,), jnp.float32, 0.2, 0.5)
    spike_indicator = jnp.any(jnp.arange(STREAM_LENGTH)[:, None] == spike_location[None, :], axis=1)
    return stable_mode + jnp.where(spike_indicator[:, None], jnp.log(1.0 - spike_surcharge)[None, :], 0.0)


def strengthened(entries, rng, source, target, shards_of, factor):
    owner, partner = [(jnp.arange(entries.shape[dim]) // (entries.shape[dim] // shards_of)).reshape([-1 if axis == dim else 1 for axis in range(entries.ndim)]) for dim in (source, target)]
    chosen = jax.random.permutation(rng, shards_of)[partner]
    strong = (owner == chosen) | (owner == (partner + shards_of // 2) % shards_of)
    return jnp.where(strong, factor * entries, entries)


def steps_of(key, shape, shards, smallest, high):
    def one(axis_at, shards_of):
        draws = jax.random.uniform(jax.random.fold_in(jax.random.fold_in(key, 6), axis_at), (shards_of,), jnp.float32, smallest / len(shards), high / len(shards))
        return jnp.repeat(jnp.exp(draws), shape[axis_at] // shards_of).reshape((-1,) + (1,) * (len(shape) - axis_at - 1))

    level = one(*shards[0])
    for cut in shards[1:]:
        level = level * one(*cut)
    return level


def deal_out(rng, own, number, rows, amount, top, bound, slope):
    ranking = jax.random.permutation(rng, amount)
    packed, common = shares(amount, rows * top, bound, slope, True), shares(amount, rows * top, bound, slope, False)
    places = jnp.arange(amount)

    def named(lengths, turn):
        used = int((lengths > 0).sum())
        fixed = max(1, used // 4)
        shifted = fixed + (places - fixed + turn * (used - fixed)) % max(1, amount - fixed)
        return jnp.zeros((amount,), jnp.int32).at[ranking[jnp.where(places < fixed, places, shifted)]].set(jnp.asarray(lengths, jnp.int32))

    lengths = jnp.where(number % 4 == 0, named(packed, number // 4), named(common, number - number // 4 - 1))
    mixed = jax.random.permutation(jax.random.fold_in(own, 3), amount)
    source_of, receiver = mixed[0:amount // 2 * 2:2], mixed[1:amount // 2 * 2:2]
    margin = jnp.minimum(lengths[source_of] - 1, bound - lengths[receiver]) // 2
    margin = jnp.where((source_of == ranking[0]) | (receiver == ranking[0]) | (lengths[receiver] == 0), 0, jnp.maximum(margin, 0))
    shifted = jax.random.randint(jax.random.fold_in(own, 4), (amount // 2,), 0, 1 << 20) % (margin + 1)
    lengths = lengths.at[source_of].add(-shifted).at[receiver].add(shifted)
    labels = jnp.searchsorted(jnp.cumsum(lengths), jnp.arange(rows * top), side="right").astype(jnp.int32)
    listing = labels.reshape(top, rows).T
    listing = listing[jax.random.permutation(jax.random.fold_in(own, 1), rows)]
    turn = jax.random.randint(jax.random.fold_in(own, 2), (rows, 1), 0, top)
    return jnp.take_along_axis(listing, (jnp.arange(top)[None, :] + turn) % top, axis=1)


def shares(number_of, total, limit, skew, full):
    portions = [(1 << 20) // math.isqrt(grade ** skew) + 1 for grade in range(1, number_of + 1)]
    largest = limit if full else min(limit, max(-(-total // number_of), total * portions[0] // sum(portions)))
    least = 1 if total - largest >= number_of - 1 else 0
    holding, spare = [largest] + [least] * (number_of - 1), total - largest - least * (number_of - 1)
    while spare > 0:
        free = [i for i in range(1, number_of) if holding[i] < largest] or [i for i in range(1, number_of) if holding[i] < limit]
        whole, left = sum([portions[i] for i in free]), spare
        for i in free:
            more = min(limit - holding[i], max(1, left * portions[i] // whole), spare)
            holding[i] = holding[i] + more
            spare = spare - more
    return np.array(holding)


def normal_values(key, shape, spread, limit, shards=(), kind=jnp.bfloat16):
    loudness = steps_of(key, shape, shards, -0.22, 0.18) if shards else 1.0
    values = jax.random.normal(key, shape, jnp.float32) * spread * loudness
    return jnp.minimum(jnp.maximum(values, -limit), limit).astype(kind)


def noise_with(key, dims, scale, reach, shards, heavy, kind=jnp.bfloat16):
    result = scale * jax.random.normal(key, dims, jnp.float32)
    if shards:
        result = result * steps_of(key, dims, shards, -0.22, 0.18)
    return jnp.clip(strengthened(result, jax.random.fold_in(key, 3), *heavy), -reach, reach).astype(kind)


def setup_inputs(seed: int = 0) -> dict:
    splits = jax.random.split(jax.random.key(seed), 14)
    queries = normal_values(splits[0], (STREAM_LENGTH, HEADS * DK), 0.125, 0.75, ((0, 8), (1, 4)))
    key_vectors = normal_values(splits[1], (STREAM_LENGTH, HEADS * DK), 0.125, 0.75, ((0, 8), (1, 4)))
    values_in = normal_values(splits[2], (STREAM_LENGTH, HEADS * DV), 0.125, 0.75, ((0, 8), (1, 4)))
    log_decay = draw_log_decay(jax.random.fold_in(splits[13], 71), 0)
    mixed_heads = normal_values(splits[4], (STREAM_LENGTH, HEADS * DV), 1.0, 6.0, ((0, 8), (1, 4)))
    out_proj = normal_values(splits[5], (HEADS * DV, D), (HEADS * DV) ** -0.5, 0.125, ((0, 4),))
    layer_input = normal_values(splits[6], (STREAM_LENGTH, D), 1.0, 6.0, ((0, 8),))
    cotangent = noise_with(splits[7], (STREAM_LENGTH, D), 1.0, 6.0, ((0, 8),), (0, 1, 8, 2.0))
    routes_keys = jax.random.split(jax.random.fold_in(splits[8], 1), STREAM_LENGTH // TOK_DEV)
    routes_turns = jax.random.permutation(jax.random.fold_in(splits[8], 3), STREAM_LENGTH // TOK_DEV)
    routes = jax.vmap(lambda own, number: deal_out(jax.random.fold_in(splits[8], 2), own, number, TOK_DEV, EXPERTS, TOP, CAP, 2))(routes_keys, routes_turns).reshape((STREAM_LENGTH, TOP))
    route_weight = jnp.clip(jnp.exp(math.log(2.0) - 2.0794415 * jax.random.uniform(splits[9], (STREAM_LENGTH, TOP), jnp.float32) ** steps_of(splits[9], (STREAM_LENGTH, TOP), ((0, 8),), -0.2, 0.2)), 0.25, 2.0)
    gate_weight = normal_values(splits[10], (EXPERTS, D, FE), D ** -0.5, 0.125, ((0, 8), (2, 4)))
    up_weight = normal_values(splits[11], (EXPERTS, D, FE), D ** -0.5, 0.125, ((0, 8), (2, 4)))
    down_weight = normal_values(splits[12], (EXPERTS, FE, D), FE ** -0.5, 0.1875, ((0, 8), (1, 4)))
    return dict(queries=queries, key_vectors=key_vectors, values_in=values_in, log_decay=log_decay, mixed_heads=mixed_heads, out_proj=out_proj, layer_input=layer_input, cotangent=cotangent, routes=routes, route_weight=route_weight, gate_weight=gate_weight, up_weight=up_weight, down_weight=down_weight)


def local_parts(query_f, key_f, grad_f, pair, decays):
    highest = lax.Precision.HIGHEST
    sigma = query_f.shape[2] ** -0.5
    length = query_f.shape[0]
    cum = jnp.cumsum(decays, axis=0)
    total = cum[-1]
    middle = 0.5 * total
    rise = jnp.exp(cum - middle)
    fall = jnp.exp(middle - cum)
    position = jnp.arange(length, dtype=jnp.int32)
    lower = (position[:, None] >= position[None, :])[None]
    score_fwd = jnp.where(lower, jnp.einsum("thc,shc->hts", query_f * rise, key_f * fall, precision=highest), 0.0) * sigma
    score_bwd = jnp.where(lower, 0.0, jnp.einsum("thc,shc->hts", query_f * fall, key_f * rise, precision=highest)) * sigma
    pair_fwd = jnp.where(lower, pair, 0.0)
    pair_bwd = jnp.where(lower, 0.0, pair)
    query_fwd = sigma * rise * jnp.einsum("hts,shc->thc", pair_fwd, key_f * fall, precision=highest)
    query_bwd = sigma * fall * jnp.einsum("hts,shc->thc", pair_bwd, key_f * rise, precision=highest)
    key_fwd = sigma * fall * jnp.einsum("hts,thc->shc", pair_fwd, query_f * rise, precision=highest)
    key_bwd = sigma * rise * jnp.einsum("hts,thc->shc", pair_bwd, query_f * fall, precision=highest)
    value_grad = jnp.einsum("hts,thv->shv", score_fwd + score_bwd, grad_f, precision=highest)
    return query_fwd, query_bwd, key_fwd, key_bwd, value_grad, cum, total


def state_terms(query_f, key_f, value_f, grad_f, cum, total):
    highest = lax.Precision.HIGHEST
    head_part = jnp.exp(cum)
    tail = jnp.exp(total - cum)
    kv_fwd = jnp.einsum("shc,shv->hcv", key_f * tail, value_f, precision=highest)
    qo_bwd = jnp.einsum("thc,thv->hcv", query_f * tail, grad_f, precision=highest)
    qo_fwd = jnp.einsum("thc,thv->hcv", query_f * head_part, grad_f, precision=highest)
    kv_bwd = jnp.einsum("shc,shv->hcv", key_f * head_part, value_f, precision=highest)
    return jnp.exp(total), kv_fwd, qo_bwd, qo_fwd, kv_bwd


def carried(parts, states, query_f, key_f, value_f, grad_f):
    highest = lax.Precision.HIGHEST
    sigma = query_f.shape[2] ** -0.5
    query_fwd, query_bwd, key_fwd, key_bwd, value_grad, cum, total = parts
    kv_low, qo_low, qo_high, kv_high = states
    head_part = jnp.exp(cum)
    tail = jnp.exp(total - cum)
    query_fwd = query_fwd + sigma * head_part * jnp.einsum("thv,hcv->thc", grad_f, kv_low, precision=highest)
    query_bwd = query_bwd + sigma * tail * jnp.einsum("thv,hcv->thc", grad_f, kv_high, precision=highest)
    key_fwd = key_fwd + sigma * tail * jnp.einsum("shv,hcv->shc", value_f, qo_high, precision=highest)
    key_bwd = key_bwd + sigma * head_part * jnp.einsum("shv,hcv->shc", value_f, qo_low, precision=highest)
    value_grad = value_grad + sigma * (jnp.einsum("shc,hcv->shv", key_f * tail, qo_high, precision=highest)
                                       + jnp.einsum("shc,hcv->shv", key_f * head_part, qo_low, precision=highest))
    grad_cum = query_f * (query_fwd - query_bwd) - key_f * (key_fwd - key_bwd)
    return query_fwd + query_bwd, key_fwd + key_bwd, value_grad, grad_cum


def carry_step(carry, inputs):
    decay_all, first_term, second_term = inputs
    grown = (decay_all[..., None] * carry[0] + first_term, decay_all[..., None] * carry[1] + second_term)
    return grown, carry


def expert_grads(inputs):
    rows, cots, weights, gate_w, up_w, down_w = inputs
    pre_gate = jnp.dot(rows, gate_w, preferred_element_type=jnp.float32)
    pre_up = jnp.dot(rows, up_w, preferred_element_type=jnp.float32)
    weighted = (weights[:, None] * cots.astype(jnp.float32)).astype(jnp.bfloat16)
    d_act = jnp.dot(weighted, down_w.T, preferred_element_type=jnp.float32)
    sigmoid_gate = jax.nn.sigmoid(pre_gate)
    silu_gate = pre_gate * sigmoid_gate
    act = (silu_gate * pre_up).astype(jnp.bfloat16)
    d_gate = (d_act * pre_up * sigmoid_gate * (1.0 + pre_gate * (1.0 - sigmoid_gate))).astype(jnp.bfloat16)
    d_up = (d_act * silu_gate).astype(jnp.bfloat16)
    grad_down = jnp.dot(act.T, weighted, preferred_element_type=jnp.float32)
    grad_gate = jnp.dot(rows.T, d_gate, preferred_element_type=jnp.float32)
    grad_up = jnp.dot(rows.T, d_up, preferred_element_type=jnp.float32)
    part_width = FE // N_TP
    parts = jnp.einsum("rpf,pfd->rpd", d_gate.reshape(-1, N_TP, part_width).astype(jnp.float32),
                       gate_w.T.reshape(N_TP, part_width, D).astype(jnp.float32))
    parts = parts + jnp.einsum("rpf,pfd->rpd", d_up.reshape(-1, N_TP, part_width).astype(jnp.float32),
                               up_w.T.reshape(N_TP, part_width, D).astype(jnp.float32))
    rounded = lax.optimization_barrier(parts.astype(jnp.bfloat16))
    row_grad = jnp.sum(rounded.astype(jnp.float32), axis=1).astype(jnp.bfloat16)
    return grad_gate, grad_up, grad_down, row_grad


def reference(queries, key_vectors, values_in, log_decay, mixed_heads, out_proj, layer_input, cotangent,
              routes, route_weight, gate_weight, up_weight, down_weight):
    blocks = STREAM_LENGTH // TOK_DEV
    rows_all = blocks * CAP
    flat_route = routes.reshape(blocks, TOK_DEV * TOP)
    onehot = (flat_route[:, :, None] == jnp.arange(EXPERTS, dtype=jnp.int32)[None, None, :]).astype(jnp.int32)
    rank = jnp.sum((jnp.cumsum(onehot, axis=1) - onehot) * onehot, axis=2)
    block_id = jnp.arange(blocks, dtype=jnp.int32)[:, None]
    place = (flat_route * rows_all + block_id * CAP + rank).reshape(-1).astype(jnp.int32)
    token_id = jnp.arange(STREAM_LENGTH * TOP, dtype=jnp.int32) // TOP
    slot_token = jnp.zeros((EXPERTS * rows_all,), jnp.int32).at[place].set(token_id)
    filled = jnp.zeros((EXPERTS * rows_all,), jnp.float32).at[place].set(1.0)
    slot_weight = jnp.zeros((EXPERTS * rows_all,), jnp.float32).at[place].set(route_weight.reshape(-1))
    expert_rows = (layer_input[slot_token].astype(jnp.float32) * filled[:, None]).astype(jnp.bfloat16)
    expert_cot = (cotangent[slot_token].astype(jnp.float32) * filled[:, None]).astype(jnp.bfloat16)
    grad_gate, grad_up, grad_down, row_grad = lax.map(expert_grads, (
        expert_rows.reshape(EXPERTS, rows_all, D), expert_cot.reshape(EXPERTS, rows_all, D),
        slot_weight.reshape(EXPERTS, rows_all), gate_weight, up_weight, down_weight))
    back = row_grad.reshape(EXPERTS * rows_all, D)[place].reshape(STREAM_LENGTH, TOP, D)
    token_grad = (cotangent.astype(jnp.float32) + jnp.sum(back.astype(jnp.float32), axis=1)).astype(jnp.bfloat16)
    grad_proj = jnp.dot(token_grad.T, mixed_heads, preferred_element_type=jnp.float32)
    head_grad = jnp.dot(token_grad, out_proj.T, preferred_element_type=jnp.float32)

    highest = lax.Precision.HIGHEST
    query_f = queries.astype(jnp.float32).reshape(blocks, TOK_DEV, HEADS, DK)
    key_f = key_vectors.astype(jnp.float32).reshape(blocks, TOK_DEV, HEADS, DK)
    value_f = values_in.astype(jnp.float32).reshape(blocks, TOK_DEV, HEADS, DV)
    grad_f = head_grad.reshape(blocks, TOK_DEV, HEADS, DV)
    decays = log_decay.reshape(blocks, TOK_DEV, HEADS, DK)
    pair = jnp.einsum("bthv,bshv->bhts", grad_f, value_f, precision=highest)
    parts = jax.vmap(local_parts)(query_f, key_f, grad_f, pair, decays)
    terms = jax.vmap(state_terms)(query_f, key_f, value_f, grad_f, parts[5], parts[6])
    zeros = jnp.zeros((HEADS, DK, DV), jnp.float32)
    _, low = lax.scan(carry_step, (zeros, zeros), (terms[0], terms[1], terms[2]))
    _, high = lax.scan(carry_step, (zeros, zeros), (terms[0], terms[3], terms[4]), reverse=True)
    query_grad, key_grad, value_grad, grad_cum = jax.vmap(carried)(
        parts, (low[0], low[1], high[0], high[1]), query_f, key_f, value_f, grad_f)
    grad_cum = grad_cum.reshape(STREAM_LENGTH, HEADS * DK)
    grad_decay = jnp.flip(jnp.cumsum(jnp.flip(grad_cum, 0), axis=0), 0)
    return (grad_gate, grad_up, grad_down, grad_proj, query_grad.reshape(STREAM_LENGTH, HEADS * DK),
            key_grad.reshape(STREAM_LENGTH, HEADS * DK), value_grad.reshape(STREAM_LENGTH, HEADS * DV), grad_decay)
```

```python
import functools

import jax
import jax.numpy as jnp
from jax import lax
from jax.experimental import pallas as pl
from jax.experimental.pallas import tpu as pltpu
from jax.sharding import PartitionSpec as P

DK = 128
DV = 256
VMEM = pltpu.VMEM
ANY = pl.ANY


def remote(source, target, send_sem, recv_sem, device):
    return pltpu.make_async_remote_copy(
        src_ref=source,
        dst_ref=target,
        send_sem=send_sem,
        recv_sem=recv_sem,
        device_id=device,
        device_id_type=pl.DeviceIdType.MESH,
    )


def greet(seq, tensor, s, tp_peers):
    barrier = pltpu.get_barrier_semaphore()
    for d in range(1, seq):
        pl.semaphore_signal(
            barrier,
            inc=1,
            device_id={"sp": lax.rem(s + d, seq)},
            device_id_type=pl.DeviceIdType.MESH,
        )
    for peer in tp_peers:
        pl.semaphore_signal(
            barrier, inc=1, device_id={"tp": peer}, device_id_type=pl.DeviceIdType.MESH
        )
    pl.semaphore_wait(barrier, seq - 1 + len(tp_peers))


def neighbours(tensor):
    t = lax.axis_index("tp")
    beside = t + 1 - 2 * lax.rem(t, 2)
    across = lax.rem(t + tensor // 2, tensor)
    return t, beside, across


class Chain:
    def __init__(self, seq, own, own_over, out, send_sem, recv_sem):
        s = lax.axis_index("sp")
        side = lax.rem(s, 2)
        line = lax.div(s, 2)
        other = s + 1 - 2 * side
        self.half = half = seq // 2

        def has(way, j):
            return line >= j if way == 0 else line + j < half

        def block(way, j):
            return s - 2 * j if way == 0 else s + 2 * j

        def relay(way, i):
            source = out.at[block(way, i)] if i else own(way)
            return remote(
                source, out.at[block(way, i)], send_sem.at[way, i], recv_sem.at[way, i],
                {"sp": s + 2 - 4 * way},
            )

        def landed(way, j):
            spot = out.at[block(way, j)]
            return remote(
                spot, spot, send_sem.at[way, j - 1], recv_sem.at[way, j - 1],
                {"sp": s - 2 + 4 * way},
            )

        def over(way, j):
            source = out.at[block(way, j)] if j else own_over
            return remote(
                source, out.at[block(way, j)], send_sem.at[2 + way, j], recv_sem.at[2 + way, j],
                {"sp": other},
            )

        self.has, self.relay, self.landed, self.over = has, relay, landed, over

    def start(self):
        for way in range(2):
            @pl.when(self.has(1 - way, 1))
            def _():
                self.relay(way, 0).start()
        self.over(0, 0).start()

    def step(self, j):
        for way in range(2):
            @pl.when(self.has(way, j))
            def _():
                self.landed(way, j).wait_recv()
                if j < self.half - 1:
                    @pl.when(self.has(1 - way, 1))
                    def _():
                        self.relay(way, j).start()
                self.over(way, j).start()

    def finish(self):
        for way in range(2):
            for j in range(self.half):
                if j < self.half - 1:
                    @pl.when(self.has(1 - way, 1) & self.has(way, j))
                    def _():
                        self.relay(way, j).wait_send()
                if j or way == 0:
                    @pl.when(self.has(way, j))
                    def _():
                        self.over(way, j).wait()


def halved(value):
    high = value.astype(jnp.bfloat16)
    return high, (value - high.astype(jnp.float32)).astype(jnp.bfloat16)


def outer(left, right):
    return lax.dot_general(
        left, right, (((0,), (0,)), ((), ())), preferred_element_type=jnp.float32
    )


def across_rows(left, right):
    return lax.dot_general(
        left, right, (((1,), (1,)), ((), ())), preferred_element_type=jnp.float32
    )


def whole_kernel(
    seq,
    tensor,
    width,
    input_ref,
    cot_ref,
    meta_ref,
    slot_ref,
    mixed_ref,
    query_ref,
    key_ref,
    value_ref,
    decay_ref,
    gate_in,
    up_in,
    down_in,
    proj_in,
    rows_out,
    cot_out,
    dgate_out,
    dup_out,
    act_out,
    mixed_out,
    total_out,
    kv_out,
    qo_out,
    token_out,
    head_out,
    cum_out,
    own_out,
    rows_all,
    cots_all,
    gate_ref,
    up_ref,
    down_ref,
    proj_ref,
    held,
    stage,
    notes,
    part,
    pair_in,
    cross_out,
    cross_in,
    summed,
    back,
    total,
    tokens_all,
    kv_own,
    qo_own,
    sums,
    z_send,
    z_recv,
    y_send,
    y_recv,
    tp_send,
    tp_recv,
    note_send,
    note_recv,
    pair_send,
    pair_recv,
    cross_send,
    cross_recv,
    give_send,
    give_recv,
    mix_send,
    mix_recv,
    kv_send,
    kv_recv,
    qo_send,
    qo_recv,
    tok_send,
    tok_recv,
    sum_send,
    sum_recv,
    sp_send,
    sp_recv,
    gather_send,
    gather_recv,
    load_sem,
    save_sem,
):
    s = lax.axis_index("sp")
    side, line = lax.rem(s, 2), lax.div(s, 2)
    other = s + 1 - 2 * side
    t, beside, across = neighbours(tensor)
    opposite = lax.rem(beside + tensor // 2, tensor)
    half = seq // 2
    bf16, f32 = jnp.bfloat16, jnp.float32
    experts, _, cap, model = rows_all.shape
    hidden = gate_ref.shape[2]
    tokens = input_ref.shape[0]
    heads = qo_out.shape[1]
    ins, outs = (input_ref, cot_ref), (rows_all, cots_all)
    loads = [
        pltpu.make_async_copy(source, target, load_sem.at[i])
        for i, (source, target) in enumerate(
            ((gate_in, gate_ref), (up_in, up_ref), (down_in, down_ref), (proj_in, proj_ref))
        )
    ]
    greet(seq, tensor, s, (beside, across))

    def columns(piece):
        return pl.ds(pl.multiple_of(piece * width, width), width)

    def place(a, block, piece):
        return outs[a].at[:, block, :, columns(piece)]

    labels = [(0, 0)] + [(way, j) for way in range(2) for j in range(1, half)]

    def number(label):
        way, j = label
        return j if way == 0 else (half - 1 + j if j else 0)

    def line_of(label):
        way, j = label
        return line - j if way == 0 else line + j

    def has(label):
        way, j = label
        return line >= j if way == 0 else line + j < half

    def ahead(way, j):
        return line + j < half if way == 0 else line >= j

    def stride(way):
        return 2 - 4 * way

    def relay(way, i, a):
        block = line_of((way, i))
        source = held.at[a, block] if i else ins[a].at[:, columns(t)]
        return remote(
            source, held.at[a, block], z_send.at[way, i, a], z_recv.at[way, i, a],
            {"sp": s + stride(way)},
        )

    def landed(way, j, a):
        spot = held.at[a, line_of((way, j))]
        return remote(
            spot, spot, z_send.at[way, j - 1, a], z_recv.at[way, j - 1, a],
            {"sp": s - stride(way)},
        )

    def note(way, j):
        return remote(
            meta_ref, notes.at[line], note_send.at[way, j], note_recv.at[way, j],
            {"sp": s + stride(way) * j},
        )

    def noted(way, j):
        spot = notes.at[line_of((way, j))]
        return remote(
            spot, spot, note_send.at[way, j], note_recv.at[way, j], {"sp": s - stride(way) * j}
        )

    def pass_on(label, a):
        k = number(label)
        return remote(
            stage.at[a, k], place(a, 2 * line_of(label) + side, t), y_send.at[a, k],
            y_recv.at[a, k], {"sp": other},
        )

    def passed(label, a):
        k = number(label)
        spot = place(a, 2 * line_of(label) + 1 - side, t)
        return remote(stage.at[a, k], spot, y_send.at[a, k], y_recv.at[a, k], {"sp": other})

    def share(way, label, mate, a):
        k = number(label)
        block = 2 * line_of(label) + (1 - side if mate else side)
        spot = place(a, block, across if way == 2 else t)
        return remote(
            spot, spot, tp_send.at[way, mate, a, k], tp_recv.at[way, mate, a, k],
            {"tp": across if way == 1 else beside},
        )

    def matching(label, group):
        table = notes[line_of(label)] if label[1] else meta_ref[...]
        row = lax.broadcasted_iota(jnp.int32, (experts * cap, tokens), 0)
        row = (row + group * (experts * cap)).astype(f32)
        first, second = table[0:1] == row, table[1:2] == row
        pick = jnp.where(first | second, 1.0, 0.0).astype(bf16)
        weight = jnp.where(first, table[2:3], 0.0) + jnp.where(second, table[3:4], 0.0)
        return pick, jnp.sum(weight, axis=1, keepdims=True)

    def rows_of(pick, weight, a, data):
        value = jnp.dot(pick, data, preferred_element_type=f32)
        value = value * weight if a else value
        return [value[e * cap : (e + 1) * cap].astype(bf16) for e in range(experts)]

    def select(label, a, mine):
        pick, weight = matching(label, s if mine else other)
        block = 2 * line_of(label) + side
        data = held[a, line_of(label)] if label[1] else ins[a][:, columns(t)]
        for e, piece in enumerate(rows_of(pick, weight, a, data)):
            if mine:
                outs[a][e, block, :, columns(t)] = piece
            else:
                stage[a, number(label), e] = piece

    def select_own(a):
        pick, weight = matching((0, 0), s)
        for piece in range(tensor):
            span = slice(piece * width, (piece + 1) * width)
            for e, rows in enumerate(rows_of(pick, weight, a, ins[a][:, span])):
                outs[a][e, s, :, span] = rows

    def z_item(j, a):
        for way in range(2):
            @pl.when(has((way, j)))
            def _():
                landed(way, j, a).wait_recv()
                if j < half - 1:
                    @pl.when(ahead(way, 1))
                    def _():
                        relay(way, j, a).start()
        for way in range(2):
            @pl.when(has((way, j)))
            def _():
                label = (way, j)
                if a == 0:
                    noted(way, j).wait_recv()
                select(label, a, False)
                pass_on(label, a).start()
                select(label, a, True)
                share(1, label, 0, a).start()
                share(0, label, 0, a).start()

    def y_item(j, a):
        for label in ((0, 0),) if j == 0 else ((0, j), (1, j)):
            @pl.when(has(label))
            def _():
                passed(label, a).wait_recv()
                share(1, label, 1, a).start()
                share(0, label, 1, a).start()

    def x_item(j, a):
        for label in ((0, 0),) if j == 0 else ((0, j), (1, j)):
            @pl.when(has(label))
            def _():
                for mate in range(2):
                    if j or mate:
                        share(1, label, mate, a).wait_recv()
                        share(2, label, mate, a).start()

    for way in range(2):
        for j in range(1, half):
            @pl.when(ahead(way, j))
            def _():
                note(way, j).start()
    for a in range(2):
        for way in range(2):
            @pl.when(ahead(way, 1))
            def _():
                relay(way, 0, a).start()
    for a in range(2):
        select((0, 0), a, False)
        pass_on((0, 0), a).start()
    for load in loads:
        load.start()
    for a in range(2):
        select_own(a)

    position = lax.broadcasted_iota(jnp.int32, (tokens, tokens), 0)
    lower = position >= lax.broadcasted_iota(jnp.int32, (tokens, tokens), 1)
    cum_out[...] = jnp.dot(
        lower.astype(f32), decay_ref[...], preferred_element_type=f32,
        precision=lax.Precision.HIGHEST,
    )

    def spans(h):
        return slice(h * DK, (h + 1) * DK), slice(h * DV, (h + 1) * DV)

    def faded(h, source):
        span, _ = spans(h)
        cum = cum_out[:, span]
        value = source[:, span].astype(f32)
        last = cum[tokens - 1 : tokens]
        return value * jnp.exp(last - cum), value * jnp.exp(cum), last

    def kv_terms(h):
        _, wide = spans(h)
        late, early, last = faded(h, key_ref)
        sums[h : h + 1] = last
        for i, value in enumerate((late, early)):
            high, low = halved(value)
            state = outer(high, value_ref[:, wide]) + outer(low, value_ref[:, wide])
            kv_own[i, h] = state.astype(bf16)
            if i == 0:
                own_out[0, h] = state

    for h in range(heads):
        kv_terms(h)

    mix = Chain(seq, lambda way: mixed_ref, mixed_ref, mixed_out, mix_send, mix_recv)
    kv = Chain(
        seq, lambda way: kv_own.at[way], kv_own.at[jnp.where(other > s, 0, 1)], kv_out,
        kv_send, kv_recv,
    )
    qo = Chain(
        seq, lambda way: qo_own.at[way], qo_own.at[jnp.where(other > s, 0, 1)], qo_out,
        qo_send, qo_recv,
    )

    def give_sum(d):
        to = lax.rem(s + d, seq)
        return remote(sums, total_out.at[s], sum_send.at[d], sum_recv.at[d], {"sp": to})

    items = [(j, a) for j in range(half) for a in range(2)]
    count = len(items)
    for n in range(2, count + 3):
        if n < count:
            z_item(*items[n])
        if n == count:
            for d in range(1, seq):
                give_sum(d).start()
            kv.start()
            mix.start()
        if n == 2:
            y_item(*items[0])
        if n - 1 < count:
            y_item(*items[n - 1])
        if n == 4:
            x_item(*items[0])
            x_item(*items[1])
        if 2 <= n - 3 < count:
            x_item(*items[n - 3])
    saves = [
        pltpu.make_async_copy(mixed_ref, mixed_out.at[s], save_sem.at[0]),
        pltpu.make_async_copy(rows_all, rows_out, save_sem.at[1]),
        pltpu.make_async_copy(cots_all, cot_out, save_sem.at[2]),
    ]
    saves[0].start()
    kv_out[s] = kv_own[0]
    total_out[s] = sums[...]
    kv.step(1)
    mix.step(1)
    for label in labels:
        @pl.when(has(label))
        def _():
            for a in range(2):
                for mate in range(2):
                    if label[1] or mate:
                        share(0, label, mate, a).wait_recv()
                        share(2, label, mate, a).wait_recv()
    saves[1].start()
    saves[2].start()
    for load in loads[:3]:
        load.wait()

    def forward_rows(e, blocks):
        shape = (len(blocks) * cap, model)
        span = slice(blocks[0], blocks[-1] + 1)
        rows = rows_all[e, span].reshape(shape)
        cots = cots_all[e, span].reshape(shape)
        gate = jnp.dot(rows, gate_ref[e], preferred_element_type=f32)
        up = jnp.dot(rows, up_ref[e], preferred_element_type=f32)
        down = across_rows(cots, down_ref[e])
        sigmoid = jax.nn.sigmoid(gate)
        silu = gate * sigmoid
        kept = (len(blocks), cap, hidden)
        act_out[e, span] = (silu * up).astype(bf16).reshape(kept)
        dgate_out[e, span] = (
            (down * up * sigmoid * (1.0 + gate * (1.0 - sigmoid))).astype(bf16).reshape(kept)
        )
        dup_out[e, span] = (down * silu).astype(bf16).reshape(kept)

    group = max(1, seq // 2) if cap % 16 == 0 else 1
    for first in range(0, seq, group):
        for e in range(experts):
            forward_rows(e, range(first, first + group))
    if half > 2:
        kv.step(2)
        mix.step(2)

    def partial(d):
        block = lax.rem(s + d, seq)
        for e in range(experts):
            for piece in range(tensor):
                span = slice(piece * width, (piece + 1) * width)
                value = across_rows(dgate_out[e, block], gate_ref[e, span])
                value += across_rows(dup_out[e, block], up_ref[e, span])
                part[e, block, :, span] = value.astype(bf16)

    def pair(d, h):
        block = lax.rem(s + d, seq)
        return remote(
            part.at[:, block, :, columns(opposite if h else beside)],
            pair_in.at[d, h],
            pair_send.at[d, h],
            pair_recv.at[d, h],
            {"tp": beside},
        )

    def cross(d):
        return remote(
            cross_out.at[d], cross_in.at[d], cross_send.at[d], cross_recv.at[d], {"tp": across}
        )

    def give(d):
        to = lax.rem(s + d, seq)
        return remote(summed.at[d], back.at[d], give_send.at[d], give_recv.at[d], {"sp": to})

    def cross_step(d):
        block = lax.rem(s + d, seq)
        pair(d, 1).wait_recv()
        for e in range(experts):
            value = part[e, block, :, columns(across)].astype(f32)
            value += pair_in[d, 1, e].astype(f32)
            cross_out[d, e] = value.astype(bf16)
        cross(d).start()

    def sum_step(d):
        block = lax.rem(s + d, seq)
        pair(d, 0).wait_recv()
        cross(d).wait_recv()
        for e in range(experts):
            value = part[e, block, :, columns(t)].astype(f32)
            value += pair_in[d, 0, e].astype(f32)
            value += cross_in[d, e].astype(f32)
            summed[d, e] = value.astype(bf16)
        if d:
            give(d).start()

    order = sorted(range(seq), key=lambda d: (d == 0, -min(d, seq - d), d))
    for i in range(seq + 3):
        if i < seq:
            partial(order[i])
            for h in (1, 0):
                pair(order[i], h).start()
        if 1 <= i <= seq:
            cross_step(order[i - 1])
        if i >= 3:
            sum_step(order[i - 3])
    for j in range(3, half):
        kv.step(j)
        mix.step(j)

    row = lax.broadcasted_iota(jnp.int32, (tokens, cap), 1)
    total[...] = cot_ref[:, columns(t)].astype(f32)
    for d in [0] + order[:-1]:
        block = lax.rem(s - d + seq, seq)
        if d:
            give(d).wait_recv()
        source = back if d else summed
        term = total[...]
        for e in range(experts):
            wanted = row + (block * experts + e) * cap
            match = (slot_ref[:, 0:1] == wanted) | (slot_ref[:, 1:2] == wanted)
            pick = jnp.where(match, 1.0, 0.0).astype(bf16)
            term += jnp.dot(pick, source[d, e], preferred_element_type=f32)
        total[...] = term
    tokens_all[:, columns(t)] = total[...].astype(bf16)

    def token(way):
        spot = tokens_all.at[:, columns(across if way == 2 else t)]
        return remote(
            spot, spot, tok_send.at[way], tok_recv.at[way],
            {"tp": across if way == 1 else beside},
        )

    token(1).start()
    token(0).start()
    loads[3].wait()
    token(1).wait_recv()
    token(2).start()
    token(0).wait_recv()
    token(2).wait_recv()

    share_span = token_out.shape[2]
    pack = share_span * seq // model
    quarter_rows = tokens // tensor

    def share_columns(to):
        return pl.ds(pl.multiple_of(lax.div(to, pack) * share_span, share_span), share_span)

    def quarter(piece):
        return pl.ds(pl.multiple_of(piece * quarter_rows, quarter_rows), quarter_rows)

    def spread(d):
        to = lax.rem(s + d, seq)
        return remote(
            tokens_all.at[quarter(t), share_columns(to)],
            token_out.at[s, quarter(t)],
            sp_send.at[d],
            sp_recv.at[d],
            {"sp": to},
        )

    def gather(d, way):
        spot = token_out.at[lax.rem(s - d + seq, seq), quarter(across if way == 2 else t)]
        return remote(
            spot, spot, gather_send.at[way, d], gather_recv.at[way, d],
            {"tp": across if way == 1 else beside},
        )

    for d in range(1, seq):
        spread(d).start()
    for h in range(heads):
        _, wide = spans(h)
        grad = across_rows(tokens_all[...], proj_ref[wide])
        head_out[:, wide] = grad
        grad_high, grad_low = halved(grad)
        late, early, _ = faded(h, query_ref)
        for i, value in enumerate((late, early)):
            high, low = halved(value)
            state = outer(high, grad_high) + outer(low, grad_high) + outer(high, grad_low)
            qo_own[i, h] = state.astype(bf16)
            if i == 0:
                own_out[1, h] = state
    qo.start()
    qo_out[s] = qo_own[0]
    token_out[s] = tokens_all[:, share_columns(s)]
    for j in range(1, half):
        qo.step(j)
    for d in range(1, seq):
        spread(d).wait_recv()
        gather(d, 1).start()
        gather(d, 0).start()
    for d in range(1, seq):
        gather(d, 1).wait_recv()
        gather(d, 2).start()

    for label in labels:
        @pl.when(has(label))
        def _():
            way, j = label
            for a in range(2):
                if j < half - 1:
                    for onto in range(2) if j == 0 else (way,):
                        @pl.when(ahead(onto, 1))
                        def _():
                            relay(onto, j, a).wait_send()
                pass_on(label, a).wait_send()
                for mate in range(2):
                    if j or mate:
                        for onto in range(3):
                            share(onto, label, mate, a).wait_send()
    for way in range(2):
        for j in range(1, half):
            @pl.when(ahead(way, j))
            def _():
                note(way, j).wait_send()
    for d in range(seq):
        for h in range(2):
            pair(d, h).wait_send()
        cross(d).wait_send()
        if d:
            give(d).wait_send()
            give_sum(d).wait()
            spread(d).wait_send()
            gather(d, 0).wait()
            gather(d, 1).wait_send()
            gather(d, 2).wait()
    for way in range(3):
        token(way).wait_send()
    for save in saves:
        save.wait()
    mix.finish()
    kv.finish()
    qo.finish()


def call(kernel, outs, in_spaces, out_spaces, scratch, number):
    return pl.pallas_call(
        kernel,
        out_shape=outs,
        in_specs=[pl.BlockSpec(memory_space=space) for space in in_spaces],
        out_specs=[pl.BlockSpec(memory_space=space) for space in out_spaces],
        scratch_shapes=scratch,
        compiler_params=pltpu.CompilerParams(collective_id=number, has_side_effects=True),
    )


def tail_sum(value):
    row = jnp.arange(value.shape[0], dtype=jnp.int32)
    mask = (row[:, None] <= row[None, :]).astype(jnp.float32)
    return jnp.tensordot(mask, value, 1, precision=lax.Precision.HIGHEST)


def local_parts(query_f, key_f, grad_f, pair, cum):
    highest = lax.Precision.HIGH
    sigma = query_f.shape[2] ** (-0.5)
    length = query_f.shape[0]
    total = cum[-1]
    middle = 0.5 * total
    rise = jnp.exp(cum - middle)
    fall = jnp.exp(middle - cum)
    position = jnp.arange(length, dtype=jnp.int32)
    lower = (position[:, None] >= position[None, :])[None]
    score_fwd = (
        jnp.where(
            lower, jnp.einsum("thc,shc->hts", query_f * rise, key_f * fall, precision=highest), 0.0
        )
        * sigma
    )
    score_bwd = (
        jnp.where(
            lower, 0.0, jnp.einsum("thc,shc->hts", query_f * fall, key_f * rise, precision=highest)
        )
        * sigma
    )
    pair_fwd = jnp.where(lower, pair, 0.0)
    pair_bwd = jnp.where(lower, 0.0, pair)
    query_fwd = sigma * rise * jnp.einsum("hts,shc->thc", pair_fwd, key_f * fall, precision=highest)
    query_bwd = sigma * fall * jnp.einsum("hts,shc->thc", pair_bwd, key_f * rise, precision=highest)
    key_fwd = sigma * fall * jnp.einsum("hts,thc->shc", pair_fwd, query_f * rise, precision=highest)
    key_bwd = sigma * rise * jnp.einsum("hts,thc->shc", pair_bwd, query_f * fall, precision=highest)
    value_grad = jnp.einsum("hts,thv->shv", score_fwd + score_bwd, grad_f, precision=highest)
    return (query_fwd, query_bwd, key_fwd, key_bwd, value_grad, cum, total)


def carried(parts, states, query_f, key_f, value_f, grad_f):
    highest = lax.Precision.HIGH
    sigma = query_f.shape[2] ** (-0.5)
    query_fwd, query_bwd, key_fwd, key_bwd, value_grad, cum, total = parts
    kv_low, qo_low, qo_high, kv_high = states
    head_part = jnp.exp(cum)
    tail = jnp.exp(total - cum)
    query_fwd = query_fwd + sigma * head_part * jnp.einsum(
        "thv,hcv->thc", grad_f, kv_low, precision=highest
    )
    query_bwd = query_bwd + sigma * tail * jnp.einsum(
        "thv,hcv->thc", grad_f, kv_high, precision=highest
    )
    key_fwd = key_fwd + sigma * tail * jnp.einsum(
        "shv,hcv->shc", value_f, qo_high, precision=highest
    )
    key_bwd = key_bwd + sigma * head_part * jnp.einsum(
        "shv,hcv->shc", value_f, qo_low, precision=highest
    )
    value_grad = value_grad + sigma * (
        jnp.einsum("shc,hcv->shv", key_f * tail, qo_high, precision=highest)
        + jnp.einsum("shc,hcv->shv", key_f * head_part, qo_low, precision=highest)
    )
    grad_cum = query_f * (query_fwd - query_bwd) - key_f * (key_fwd - key_bwd)
    return (query_fwd + query_bwd, key_fwd + key_bwd, value_grad, grad_cum)


def body(
    queries,
    key_vectors,
    values_in,
    log_decay,
    mixed_heads,
    out_proj,
    layer_input,
    cotangent,
    routes,
    route_weight,
    gate_weight,
    up_weight,
    down_weight,
):
    tokens, top = routes.shape
    seq = lax.axis_size("sp")
    tensor = lax.axis_size("tp")
    s = lax.axis_index("sp")
    experts, _, hidden = gate_weight.shape
    all_experts = experts * seq
    capacity = 2 * tokens * top // all_experts
    model = cotangent.shape[1]
    width = model // tensor
    half = seq // 2
    bf16, f32 = jnp.bfloat16, jnp.float32
    dma = pltpu.SemaphoreType.DMA

    heads = queries.shape[1] // DK
    high = lax.Precision.HIGH

    flat_route = routes.reshape(-1)
    onehot = flat_route[:, None] == jnp.arange(all_experts, dtype=jnp.int32)[None, :]
    pair_id = jnp.arange(tokens * top, dtype=jnp.int32)
    before = (pair_id[:, None] > pair_id[None, :]).astype(bf16)
    counts = jnp.dot(before, onehot.astype(bf16), preferred_element_type=f32)
    rank = jnp.sum(jnp.where(onehot, counts, 0.0), axis=1).astype(jnp.int32)
    slot = (flat_route * capacity + rank).reshape(tokens, top)
    lines = jnp.concatenate([slot.astype(f32).T, route_weight.T], axis=0)
    meta = jnp.pad(lines, ((0, 8 - 2 * top), (0, 0)))

    share = model // seq
    pack = max(1, 128 // share)
    rows_shape = (experts, seq, capacity, model)
    block_shape = (seq, experts, capacity, width)
    hidden_shape = (experts, seq, capacity, hidden)
    state_shape = (seq, heads, DK, DV)
    labels = 2 * half - 1

    def struct(shape, dtype):
        return jax.ShapeDtypeStruct(shape, dtype)

    def sems(*shape):
        return [dma(shape), dma(shape)]

    (
        expert_rows,
        weighted,
        d_gate,
        d_up,
        act,
        mixed_all,
        total_all,
        kv_all,
        qo_all,
        token_all,
        head_grad,
        cum_flat,
        own_states,
    ) = call(
        functools.partial(whole_kernel, seq, tensor, width),
        (
            struct(rows_shape, bf16),
            struct(rows_shape, bf16),
            struct(hidden_shape, bf16),
            struct(hidden_shape, bf16),
            struct(hidden_shape, bf16),
            struct((seq,) + mixed_heads.shape, bf16),
            struct((seq, heads, DK), f32),
            struct(state_shape, bf16),
            struct(state_shape, bf16),
            struct((seq, tokens, share * pack), bf16),
            struct((tokens, heads * DV), f32),
            struct((tokens, heads * DK), f32),
            struct((2, heads, DK, DV), f32),
        ),
        (VMEM,) * 9 + (ANY,) * 4,
        (ANY, ANY, VMEM, VMEM, VMEM, ANY) + (VMEM,) * 7,
        [
            pltpu.VMEM(rows_shape, bf16),
            pltpu.VMEM(rows_shape, bf16),
            pltpu.VMEM(gate_weight.shape, bf16),
            pltpu.VMEM(up_weight.shape, bf16),
            pltpu.VMEM(down_weight.shape, bf16),
            pltpu.VMEM(out_proj.shape, bf16),
            pltpu.VMEM((2, half, tokens, width), bf16),
            pltpu.VMEM((2, labels, experts, capacity, width), bf16),
            pltpu.VMEM((half,) + meta.shape, f32),
            pltpu.VMEM(rows_shape, bf16),
            pltpu.VMEM((seq, 2, experts, capacity, width), bf16),
            pltpu.VMEM(block_shape, bf16),
            pltpu.VMEM(block_shape, bf16),
            pltpu.VMEM(block_shape, bf16),
            pltpu.VMEM(block_shape, bf16),
            pltpu.VMEM((tokens, width), f32),
            pltpu.VMEM((tokens, model), bf16),
            pltpu.VMEM((2, heads, DK, DV), bf16),
            pltpu.VMEM((2, heads, DK, DV), bf16),
            pltpu.VMEM((heads, DK), f32),
            *sems(2, half, 2),
            *sems(2, labels),
            *sems(3, 2, 2, labels),
            *sems(2, half),
            *sems(seq, 2),
            *sems(seq),
            *sems(seq),
            *sems(4, half),
            *sems(4, half),
            *sems(4, half),
            *sems(3),
            *sems(seq),
            *sems(seq),
            *sems(3, seq),
            dma((4,)),
            dma((3,)),
        ],
        0,
    )(
        layer_input,
        cotangent,
        meta,
        slot,
        mixed_heads,
        queries,
        key_vectors,
        values_in,
        log_decay,
        gate_weight,
        up_weight,
        down_weight,
        out_proj,
    )
    flat = (experts, seq * capacity)
    expert_rows, weighted = expert_rows.reshape(flat + (model,)), weighted.reshape(flat + (model,))
    d_gate, d_up, act = (value.reshape(flat + (hidden,)) for value in (d_gate, d_up, act))
    if pack > 1:
        token_all = lax.dynamic_slice_in_dim(token_all, lax.rem(s, pack) * share, share, 2)
    grad_gate, grad_up, grad_down = (
        jnp.einsum("erd,erf->edf", expert_rows, d_gate, preferred_element_type=f32),
        jnp.einsum("erd,erf->edf", expert_rows, d_up, preferred_element_type=f32),
        jnp.einsum("erf,erd->efd", act, weighted, preferred_element_type=f32),
    )
    grad_proj = lax.dot_general(
        token_all, mixed_all, (((0, 1), (0, 1)), ((), ())), preferred_element_type=f32
    )

    query_f = queries.reshape(tokens, heads, DK).astype(f32)
    key_f = key_vectors.reshape(tokens, heads, DK).astype(f32)
    value_f = values_in.reshape(tokens, heads, DV).astype(f32)
    grad_f = head_grad.reshape(tokens, heads, DV)
    cum = cum_flat.reshape(tokens, heads, DK)
    total = cum[-1]
    kv_fwd, qo_bwd = own_states[0], own_states[1]
    pair = jnp.einsum("thv,shv->hts", grad_f, value_f, precision=high)
    parts = local_parts(query_f, key_f, grad_f, pair, cum)
    block = jnp.arange(seq, dtype=jnp.int32)
    low_span = ((block[None, :] > block[:, None]) & (block[None, :] < s)).astype(f32)
    high_span = ((block[None, :] < block[:, None]) & (block[None, :] > s)).astype(f32)

    def carry(span, mask):
        logs = jnp.sum(span[:, :, None, None] * total_all[None], axis=1)
        return jnp.where(mask[:, None, None], jnp.exp(logs), 0.0)[..., None]

    low_scale = carry(low_span, block < s)
    high_scale = carry(high_span, block > s)
    kv_low = jnp.sum(low_scale * kv_all.astype(f32), axis=0)
    kv_high = jnp.sum(high_scale * kv_all.astype(f32), axis=0)
    qo_low = jnp.sum(low_scale * qo_all.astype(f32), axis=0)
    qo_high = jnp.sum(high_scale * qo_all.astype(f32), axis=0)
    query_grad, key_grad, value_grad, grad_cum = carried(
        parts, (kv_low, qo_low, qo_high, kv_high), query_f, key_f, value_f, grad_f
    )
    decay_all = jnp.exp(total)[..., None]
    beyond = DK ** (-0.5) * jnp.sum(
        (decay_all * kv_low + kv_fwd) * qo_high + (decay_all * qo_low + qo_bwd) * kv_high, axis=2
    )
    grad_decay = tail_sum(grad_cum) + beyond[None]
    return (
        grad_gate,
        grad_up,
        grad_down,
        grad_proj,
        query_grad.reshape(tokens, heads * DK),
        key_grad.reshape(tokens, heads * DK),
        value_grad.reshape(tokens, heads * DV),
        grad_decay.reshape(tokens, heads * DK),
    )


def solution(mesh):
    return jax.shard_map(
        body,
        mesh=mesh,
        in_specs=(
            P("sp", "tp"),
            P("sp", "tp"),
            P("sp", "tp"),
            P("sp", "tp"),
            P("sp", "tp"),
            P("tp", None),
            P("sp", None),
            P("sp", None),
            P("sp", None),
            P("sp", None),
            P("sp", None, "tp"),
            P("sp", None, "tp"),
            P("sp", "tp", None),
        ),
        out_specs=(
            P("sp", None, "tp"),
            P("sp", None, "tp"),
            P("sp", "tp", None),
            P("sp", "tp"),
            P("sp", "tp"),
            P("sp", "tp"),
            P("sp", "tp"),
            P("sp", "tp"),
        ),
        check_vma=False,
    )
```
